32 devices in a mesh: ep: 16 (over z, y, x), tp: 2 (over core).
Axes of the slice: x: 2, y: 2, z: 4, core: 2. Of those that a mesh axis runs over, the one named last changes fastest.
Arguments:
- resid: bfloat16 [256, 2048], P('ep'), may hold values from -6 to 6
- proj_x: bfloat16 [256, 2048], P('ep', 'tp'), may hold values from -6 to 6
- proj_z: bfloat16 [256, 2048], P('ep', 'tp'), may hold values from -6 to 6
- proj_bc: bfloat16 [256, 2, 512], P('ep', None, 'tp'), may hold values from -6 to 6
- proj_dt: bfloat16 [256, 32], P('ep', 'tp'), may hold values from -6 to 6
- tail_x: bfloat16 [256, 3, 2048], P('ep', None, 'tp'), may hold values from -6 to 6
- tail_bc: bfloat16 [256, 3, 2, 512], P('ep', None, None, 'tp'), may hold values from -6 to 6
- taps_x: bfloat16 [4, 2048], P(None, 'tp'), may hold values from -3 to 3
- taps_bc: bfloat16 [4, 2, 512], P(None, None, 'tp'), may hold values from -3 to 3
- ssm_state: float32 [256, 32, 4096], P('ep', 'tp'), may hold values from -1.5 to 1.5
- dt_bias: float32 [32], P('tp'), may hold values from -4 to 0
- decay_log: float32 [32], P('tp'), may hold values from -1 to 2.5
- group_gain: float32 [2048], P('tp'), may hold values from 0.1 to 1.9
- out_proj: bfloat16 [2048, 2048], P('tp', 'ep'), may hold values from -0.125 to 0.125
- ffn_gain: float32 [2048], replicated, may hold values from 0.1 to 1.9
- dense_gate: bfloat16 [2048, 4096], P(None, ('ep', 'tp')), may hold values from -0.125 to 0.125
- dense_up: bfloat16 [2048, 4096], P(None, ('ep', 'tp')), may hold values from -0.125 to 0.125
- dense_down: bfloat16 [4096, 2048], P(('ep', 'tp')), may hold values from -0.09375 to 0.09375
- branch_gate: bfloat16 [2048], replicated, may hold values from -0.125 to 0.125
- group_weights: float32 [256, 4], replicated, may hold values from 0.2 to 1
- expert_ids: int32 [256, 6], replicated, may hold values from 0 to 15, all different within a row; in each aligned block of 16 rows (0 to 15, 16 to 31, ...) at most 7 rows name the same one
- expert_weights: float32 [256, 6], replicated, may hold values from 0.1 to 1
- exp_gate: bfloat16 [16, 2048, 512], P('ep', None, 'tp'), may hold values from -0.125 to 0.125
- exp_up: bfloat16 [16, 2048, 512], P('ep', None, 'tp'), may hold values from -0.125 to 0.125
- exp_down: bfloat16 [16, 512, 2048], P('ep', 'tp'), may hold values from -0.25 to 0.25
Outputs:
- out: bfloat16 [256, 2048], P(('ep', 'tp'))
- new_state: float32 [256, 32, 4096], P('ep', 'tp')
The draws below stay inside these ranges and needn't reach their ends.
Inputs may be any that keep to these rules, and one draw needn't show every extreme that they name: `expert_ids`: each row names 6 different experts. In the rows of one index of ep (aligned blocks of 16 rows) no expert is named more than 7 times, a bound that some block reaches.
All inputs are finite; a program needn't handle non-finite values.
Results may differ from the reference program's by a relative error of at most 0.013.
Values may be sent and summed in bfloat16 or wider, within the bound.
A program may use at most 128 MiB of HBM per device.

```python
import math
import jax
import jax.numpy as jnp
import numpy as np
from jax import lax

D = 2048
HEADS = 32
HEAD_P = 64
NSTATE = 64
BC_GROUPS = 8
TAPS = 4
EFF = 512
DFF = 4096
GROUPS = 4
TOPK = 6
SEQ_DEV = 16
INNER = 2048
HPG = 4
BATCH = 256
EXPERTS = 16
EPG = 4
CAP = 7


def block_scale(own_key, dims, shards, smallest, largest):
    gain, own = 1.0, jax.random.fold_in(own_key, 6)
    for dim, parts in shards:
        steps = jnp.exp(jax.random.uniform(jax.random.fold_in(own, dim), (parts,), jnp.float32, smallest / len(shards), largest / len(shards)))
        gain = gain * jnp.repeat(steps, dims[dim] // parts).reshape([-1 if axis == dim else 1 for axis in range(len(dims))])
    return gain


def shared_out(own_key, own, number, rows, count, top, most, slope):
    sequence = jax.random.permutation(own_key, count)
    crowded, common = portions_of(count, rows * top, most, slope, True), portions_of(count, rows * top, most, slope, False)
    places = jnp.arange(count)

    def named(lengths, offset_by):
        used = int((lengths > 0).sum())
        fixed = max(1, used // 4)
        shifted = fixed + (places - fixed + offset_by * (used - fixed)) % max(1, count - fixed)
        return jnp.zeros((count,), jnp.int32).at[sequence[jnp.where(places < fixed, places, shifted)]].set(jnp.asarray(lengths, jnp.int32))

    lengths = jnp.where(number % 4 == 0, named(crowded, number // 4), named(common, number - number // 4 - 1))
    mixed = jax.random.permutation(jax.random.fold_in(own, 3), count)
    donor, receiver = mixed[0:count // 2 * 2:2], mixed[1:count // 2 * 2:2]
    room = jnp.minimum(lengths[donor] - 1, most - lengths[receiver]) // 2
    room = jnp.where((donor == sequence[0]) | (receiver == sequence[0]) | (lengths[receiver] == 0), 0, jnp.maximum(room, 0))
    shifted = jax.random.randint(jax.random.fold_in(own, 4), (count // 2,), 0, 1 << 20) % (room + 1)
    lengths = lengths.at[donor].add(-shifted).at[receiver].add(shifted)
    members = jnp.searchsorted(jnp.cumsum(lengths), jnp.arange(rows * top), side="right").astype(jnp.int32)
    table = members.reshape(top, rows).T
    table = table[jax.random.permutation(jax.random.fold_in(own, 1), rows)]
    offset_by = jax.random.randint(jax.random.fold_in(own, 2), (rows, 1), 0, top)
    return jnp.take_along_axis(table, (jnp.arange(top)[None, :] + offset_by) % top, axis=1)


def portions_of(count, total, limit, lean, full):
    loads = [(1 << 20) // math.isqrt(standing ** lean) + 1 for standing in range(1, count + 1)]
    largest = limit if full else min(limit, max(-(-total // count), total * loads[0] // sum(loads)))
    least = 1 if total - largest >= count - 1 else 0
    holding, rest = [largest] + [least] * (count - 1), total - largest - least * (count - 1)
    while rest > 0:
        free = [i for i in range(1, count) if holding[i] < largest] or [i for i in range(1, count) if holding[i] < limit]
        whole, left = sum([loads[i] for i in free]), rest
        for i in free:
            addition = min(limit - holding[i], max(1, left * loads[i] // whole), rest)
            holding[i] = holding[i] + addition
            rest = rest - addition
    return np.array(holding)


def gaussian(stream_key, dims, scale, most, cuts=(), kind=jnp.bfloat16):
    drawn = jax.random.normal(stream_key, dims, jnp.float32) * scale
    if len(cuts) > 0:
        drawn = block_scale(stream_key, dims, cuts, -0.22, 0.18) * drawn
    return jnp.clip(drawn, min=-most, max=most).astype(kind)


def setup_inputs(seed: int = 0) -> dict:
    key_of = jax.random.split(jax.random.key(seed), 26)
    resid = gaussian(key_of[0], (BATCH, D), 1.0, 6.0, ((0, 16),))
    proj_x = gaussian(key_of[1], (BATCH, INNER), 1.0, 6.0, ((0, 16), (1, 2)))
    proj_z = gaussian(key_of[2], (BATCH, INNER), 1.0, 6.0, ((0, 16), (1, 2)))
    proj_bc = gaussian(key_of[3], (BATCH, 2, BC_GROUPS * NSTATE), 1.0, 6.0, ((0, 16), (2, 2)))
    proj_dt = gaussian(key_of[4], (BATCH, HEADS), 1.0, 6.0, ((0, 16), (1, 2)))
    tail_x = gaussian(key_of[5], (BATCH, TAPS - 1, INNER), 1.0, 6.0, ((0, 16), (2, 2)))
    tail_bc = gaussian(key_of[6], (BATCH, TAPS - 1, 2, BC_GROUPS * NSTATE), 1.0, 6.0, ((0, 16), (3, 2)))
    taps_x = gaussian(key_of[7], (TAPS, INNER), TAPS ** -0.5, 3.0, ((1, 2),))
    taps_bc = gaussian(key_of[8], (TAPS, 2, BC_GROUPS * NSTATE), TAPS ** -0.5, 3.0, ((2, 2),))
    ssm_state = gaussian(key_of[9], (BATCH, HEADS, HEAD_P * NSTATE), 0.25, 1.5, ((0, 16), (1, 2)), jnp.float32)
    dt_bias = jnp.clip(-4.0 + 4.0 * jax.random.uniform(key_of[10], (HEADS,), jnp.float32) ** block_scale(key_of[10], (HEADS,), ((0, 2),), -0.2, 0.2), -4.0, 0.0)
    decay_log = jnp.clip(-1.0 + 3.5 * jax.random.uniform(key_of[11], (HEADS,), jnp.float32) ** block_scale(key_of[11], (HEADS,), ((0, 2),), -0.2, 0.2), -1.0, 2.5)
    group_gain = jnp.clip(1.0 + 0.18 * jax.random.normal(key_of[12], (INNER,), jnp.float32), 0.1, 1.9)
    out_proj = gaussian(key_of[13], (INNER, D), INNER ** -0.5, 0.125, ((0, 2), (1, 16)))
    ffn_gain = jnp.clip(1.0 + 0.18 * jax.random.normal(key_of[14], (D,), jnp.float32), 0.1, 1.9)
    dense_gate = gaussian(key_of[15], (D, DFF), D ** -0.5, 0.125, ((1, 32),))
    dense_up = gaussian(key_of[16], (D, DFF), D ** -0.5, 0.125, ((1, 32),))
    dense_down = gaussian(key_of[17], (DFF, D), DFF ** -0.5, 0.09375, ((0, 32),))
    branch_gate = gaussian(key_of[18], (D,), D ** -0.5, 0.125)
    group_weights = jnp.clip(jnp.exp(jax.random.uniform(key_of[19], (BATCH, GROUPS), jnp.float32, math.log(0.2), math.log(1.0))), 0.2, 1.0)
    expert_ids_keys = jax.random.split(jax.random.fold_in(key_of[20], 1), BATCH // SEQ_DEV)
    expert_ids_turns = jax.random.permutation(jax.random.fold_in(key_of[20], 3), BATCH // SEQ_DEV)
    expert_ids = jax.vmap(lambda own, number: shared_out(jax.random.fold_in(key_of[20], 2), own, number, SEQ_DEV, EXPERTS, TOPK, CAP, 2))(expert_ids_keys, expert_ids_turns).reshape((BATCH, TOPK))
    expert_weights = jnp.clip(jnp.exp(jax.random.uniform(key_of[21], (BATCH, TOPK), jnp.float32, math.log(0.1), math.log(1.0))), 0.1, 1.0)
    exp_gate = gaussian(key_of[22], (EXPERTS, D, EFF), D ** -0.5, 0.125, ((0, 16), (2, 2)))
    exp_up = gaussian(key_of[23], (EXPERTS, D, EFF), D ** -0.5, 0.125, ((0, 16), (2, 2)))
    exp_down = gaussian(key_of[24], (EXPERTS, EFF, D), EFF ** -0.5, 0.25, ((0, 16), (1, 2)))
    return {"resid": resid, "proj_x": proj_x, "proj_z": proj_z, "proj_bc": proj_bc, "proj_dt": proj_dt, "tail_x": tail_x, "tail_bc": tail_bc, "taps_x": taps_x, "taps_bc": taps_bc, "ssm_state": ssm_state, "dt_bias": dt_bias, "decay_log": decay_log, "group_gain": group_gain, "out_proj": out_proj, "ffn_gain": ffn_gain, "dense_gate": dense_gate, "dense_up": dense_up, "dense_down": dense_down, "branch_gate": branch_gate, "group_weights": group_weights, "expert_ids": expert_ids, "expert_weights": expert_weights, "exp_gate": exp_gate, "exp_up": exp_up, "exp_down": exp_down}


EPSILON = 1e-06

def state_update(proj_x, proj_z, proj_bc, proj_dt, tail_x, tail_bc, taps_x, taps_bc, ssm_state, dt_bias, decay_log, group_gain):
    window_x = jnp.concatenate([tail_x, proj_x[:, None]], axis=1).astype(jnp.float32)
    conv_x = jax.nn.silu(lax.optimization_barrier(jnp.sum(window_x * taps_x.astype(jnp.float32)[None], axis=1)))
    window_bc = jnp.concatenate([tail_bc, proj_bc[:, None]], axis=1).astype(jnp.float32)
    conv_bc = jax.nn.silu(lax.optimization_barrier(jnp.sum(window_bc * taps_bc.astype(jnp.float32)[None], axis=1)))
    count = proj_x.shape[0]
    heads = proj_dt.shape[1]
    x_heads = conv_x.reshape(count, heads, HEAD_P)
    grouped_bc = conv_bc.reshape(count, 2, heads // HPG, NSTATE)
    input_heads = jnp.repeat(grouped_bc[:, 0], HPG, axis=1)
    read_heads = jnp.repeat(grouped_bc[:, 1], HPG, axis=1)
    step_size = jax.nn.softplus(proj_dt.astype(jnp.float32) + dt_bias)
    decay = jnp.exp(-step_size * jnp.exp(decay_log))
    state = ssm_state.reshape(count, heads, HEAD_P, NSTATE)
    fresh = (step_size[:, :, None] * x_heads)[:, :, :, None] * input_heads[:, :, None, :]
    new_state = decay[:, :, None, None] * state + fresh
    readout = lax.optimization_barrier(jnp.sum(new_state * read_heads[:, :, None, :], axis=-1))
    gated = readout.reshape(count, heads * HEAD_P) * jax.nn.silu(proj_z.astype(jnp.float32))
    grouped = gated.reshape(count, heads // HPG, HPG * HEAD_P)
    grouped = grouped * lax.rsqrt(lax.optimization_barrier(jnp.mean(grouped * grouped, axis=-1, keepdims=True)) + EPSILON)
    y_out = (grouped.reshape(count, heads * HEAD_P) * group_gain).astype(jnp.bfloat16)
    return (y_out, new_state.reshape(count, heads, HEAD_P * NSTATE))

def expert_slots(expert_ids, expert_weights, group_weights, index, experts, group_size, capacity):
    batch = expert_ids.shape[0]
    rows_each = batch // experts
    pairs = rows_each * TOPK
    pick = (jnp.arange(GROUPS, dtype=jnp.int32) == index // group_size).astype(jnp.float32)
    coarse = lax.optimization_barrier(jnp.sum(group_weights * pick[None], axis=1))
    pair_weight = (expert_weights * coarse[:, None]).reshape(experts, pairs)
    hits = (expert_ids.reshape(experts, pairs) == index).astype(jnp.int32)
    ranks = jnp.cumsum(hits, axis=1, dtype=jnp.int32)
    levels = jnp.arange(1, capacity + 1, dtype=jnp.int32)
    select = hits[:, None, :] * (ranks[:, None, :] == levels[None, :, None]).astype(jnp.int32)
    pair_row = jnp.arange(pairs, dtype=jnp.int32) // TOPK
    local_row = lax.optimization_barrier(jnp.sum(select * pair_row[None, None, :], axis=-1, dtype=jnp.int32))
    filled = lax.optimization_barrier(jnp.sum(select, axis=-1, dtype=jnp.int32)).reshape(-1)
    slot_weight = lax.optimization_barrier(jnp.sum(select.astype(jnp.float32) * pair_weight[:, None, :], axis=-1)).reshape(-1)
    row_index = (local_row + jnp.arange(experts, dtype=jnp.int32)[:, None] * rows_each).reshape(-1)
    return (row_index, filled, slot_weight)

def reference(resid, proj_x, proj_z, proj_bc, proj_dt, tail_x, tail_bc, taps_x, taps_bc, ssm_state, dt_bias, decay_log, group_gain, out_proj, ffn_gain, dense_gate, dense_up, dense_down, branch_gate, group_weights, expert_ids, expert_weights, exp_gate, exp_up, exp_down):
    y_out, new_state = state_update(proj_x, proj_z, proj_bc, proj_dt, tail_x, tail_bc, taps_x, taps_bc, ssm_state, dt_bias, decay_log, group_gain)
    mixed = jnp.dot(y_out, out_proj, preferred_element_type=jnp.float32)
    resid_new = (resid.astype(jnp.float32) + mixed).astype(jnp.bfloat16)
    widened = resid_new.astype(jnp.float32)
    normed = (widened * lax.rsqrt(lax.optimization_barrier(jnp.mean(widened * widened, axis=-1, keepdims=True)) + EPSILON) * ffn_gain).astype(jnp.bfloat16)
    score = jnp.dot(normed, branch_gate, preferred_element_type=jnp.float32)
    dense_pre = jnp.dot(normed, dense_gate, preferred_element_type=jnp.float32)
    dense_lin = jnp.dot(normed, dense_up, preferred_element_type=jnp.float32)
    dense_hidden = (jax.nn.sigmoid(score)[:, None] * jax.nn.silu(dense_pre) * dense_lin).astype(jnp.bfloat16)
    total = jnp.dot(dense_hidden, dense_down, preferred_element_type=jnp.float32)

    def expert_step(accum, items):
        gate_w, up_w, down_w, index = items
        row_index, filled, slot_weight = expert_slots(expert_ids, expert_weights, group_weights, index, EXPERTS, EPG, CAP)
        slot_rows = jnp.take(normed, row_index, axis=0)
        slot_pre = jnp.dot(slot_rows, gate_w, preferred_element_type=jnp.float32)
        slot_lin = jnp.dot(slot_rows, up_w, preferred_element_type=jnp.float32)
        slot_hidden = (slot_weight[:, None] * jax.nn.silu(slot_pre) * slot_lin).astype(jnp.bfloat16)
        slot_out = jnp.dot(slot_hidden, down_w, preferred_element_type=jnp.float32)
        slot_out = slot_out * (filled > 0).astype(jnp.float32)[:, None]
        return (accum.at[row_index].add(slot_out), None)
    total, _ = lax.scan(expert_step, total, (exp_gate, exp_up, exp_down, jnp.arange(EXPERTS, dtype=jnp.int32)))
    out = (widened + total).astype(jnp.bfloat16)
    return (out, new_state)
```

```python
import functools

import jax
import jax.numpy as jnp
from jax import lax
from jax.experimental import pallas as pl
from jax.experimental.pallas import tpu as pltpu
from jax.sharding import PartitionSpec as P

HEAD_P = 64
NSTATE = 64
GROUPS = 4
TOPK = 6
HPG = 4


EPSILON = 1e-06
LANES = 512
PLANE = 4
MESH = pl.DeviceIdType.MESH
F32 = jnp.float32
BF16 = jnp.bfloat16


def mm(a, b):
    return jnp.dot(a, b, preferred_element_type=F32)


def iota(shape, dim):
    return lax.broadcasted_iota(jnp.int32, shape, dim)


def one_hot(cond):
    return cond.astype(F32).astype(BF16)


def state_kernel(
    x_ref, z_ref, inp_ref, rd_ref, dt_ref, bias_ref, log_ref, gain_ref, state_ref,
    y_ref, new_ref, xs, inp_s, rd_s, decay_s, acc,
):
    j = pl.program_id(0)
    count, heads = dt_ref.shape
    rows = count * heads
    inner = heads * HEAD_P
    groups = heads // HPG

    def head_mask(lanes, per):
        head = lax.rem(iota((rows, lanes), 0), heads)
        return head // (HPG if per == groups else 1) == iota((rows, lanes), 1) // (lanes // per)

    @pl.when(j == 0)
    def _():
        spread = one_hot(iota((rows, count), 0) // heads == iota((rows, count), 1))
        dt = mm(spread, dt_ref[...])
        step = jax.nn.softplus(dt + bias_ref[...])
        decay = jnp.exp(-step * jnp.exp(log_ref[...]))
        own = head_mask(heads, heads)
        step_col = jnp.sum(jnp.where(own, step, 0.0), axis=1, keepdims=True)
        decay_s[...] = jnp.sum(jnp.where(own, decay, 0.0), axis=1, keepdims=True)
        xr = mm(spread, x_ref[...].astype(BF16))
        xr = jnp.where(head_mask(inner, heads), xr, 0.0).astype(BF16)
        fold = one_hot(lax.rem(iota((inner, HEAD_P), 0), HEAD_P) == iota((inner, HEAD_P), 1))
        xs[...] = mm(xr, fold).astype(BF16)
        width = groups * NSTATE
        gmask = head_mask(width, groups)
        twice = one_hot(
            lax.rem(iota((width, 2 * NSTATE), 0), NSTATE)
            == lax.rem(iota((width, 2 * NSTATE), 1), NSTATE)
        )
        ir = jnp.where(gmask, mm(spread, inp_ref[...].astype(BF16)), 0.0).astype(BF16)
        inp_s[...] = mm(ir, twice) * step_col
        rr = jnp.where(gmask, mm(spread, rd_ref[...].astype(BF16)), 0.0).astype(BF16)
        rd_s[...] = mm(rr, twice)
        acc[...] = jnp.zeros_like(acc)

    lanes = state_ref.shape[1]
    tiles = lanes // (2 * NSTATE)
    expand = one_hot(
        iota((HEAD_P, lanes), 0) == (iota((HEAD_P, lanes), 1) + j * lanes) // NSTATE
    )
    collect = one_hot(
        iota((lanes, HEAD_P), 1) == (iota((lanes, HEAD_P), 0) + j * lanes) // NSTATE
    )
    fresh = mm(xs[...], expand) * jnp.concatenate([inp_s[...]] * tiles, axis=1)
    new = decay_s[...] * state_ref[...] + fresh
    new_ref[...] = new
    prod = (new * jnp.concatenate([rd_s[...]] * tiles, axis=1)).astype(BF16)
    acc[...] += mm(prod, collect)

    @pl.when(j == pl.num_programs(0) - 1)
    def _():
        unfold = one_hot(lax.rem(iota((HEAD_P, inner), 1), HEAD_P) == iota((HEAD_P, inner), 0))
        gatherer = one_hot(iota((count, rows), 1) // heads == iota((count, rows), 0))
        mask = head_mask(inner, heads)
        high = acc[...].astype(BF16)
        low = (acc[...] - high.astype(F32)).astype(BF16)
        read = jnp.zeros((count, inner), F32)
        for piece in (high, low):
            wide = jnp.where(mask, mm(piece, unfold), 0.0).astype(BF16)
            read = read + mm(gatherer, wide)
        gated = read * jax.nn.silu(z_ref[...].astype(F32))
        size = HPG * HEAD_P
        for g in range(groups):
            cols = slice(g * size, (g + 1) * size)
            part = gated[:, cols]
            part = part * lax.rsqrt(jnp.mean(part * part, axis=-1, keepdims=True) + EPSILON)
            y_ref[:, cols] = (part * gain_ref[:, cols]).astype(BF16)


def state_step(
    proj_x, proj_z, proj_bc, proj_dt, tail_x, tail_bc, taps_x, taps_bc, ssm_state,
    dt_bias, decay_log, group_gain,
):
    window_x = jnp.concatenate([tail_x, proj_x[:, None]], axis=1).astype(F32)
    conv_x = jax.nn.silu(jnp.sum(window_x * taps_x.astype(F32)[None], axis=1))
    window_bc = jnp.concatenate([tail_bc, proj_bc[:, None]], axis=1).astype(F32)
    conv_bc = jax.nn.silu(jnp.sum(window_bc * taps_bc.astype(F32)[None], axis=1))
    count, heads, width = ssm_state.shape
    rows = count * heads
    full = lambda a: pl.BlockSpec(a.shape, lambda j: (0,) * a.ndim)
    small = (
        conv_x, proj_z, conv_bc[:, 0], conv_bc[:, 1], proj_dt,
        dt_bias[None], decay_log[None], group_gain[None],
    )
    block = pl.BlockSpec((rows, LANES), lambda j: (0, j))
    y_out, new_state = pl.pallas_call(
        state_kernel,
        grid=(width // LANES,),
        in_specs=[full(a) for a in small] + [block],
        out_specs=[pl.BlockSpec((count, heads * HEAD_P), lambda j: (0, 0)), block],
        out_shape=[
            jax.ShapeDtypeStruct((count, heads * HEAD_P), BF16),
            jax.ShapeDtypeStruct((rows, width), F32),
        ],
        scratch_shapes=[
            pltpu.VMEM((rows, HEAD_P), BF16),
            pltpu.VMEM((rows, 2 * NSTATE), F32),
            pltpu.VMEM((rows, 2 * NSTATE), F32),
            pltpu.VMEM((rows, 1), F32),
            pltpu.VMEM((rows, HEAD_P), F32),
        ],
        name="state_step",
    )(*small, ssm_state.reshape(rows, width))
    return y_out, new_state.reshape(count, heads, width)


def layer_kernel(
    y_ref, resid_ref, gain_ref, bgate_ref, gw_ref, ids_ref, ew_ref,
    oproj_hbm, dg_hbm, du_hbm, dd_hbm, eg_hbm, eu_hbm, ed_hbm,
    out_ref,
    oproj, dg, du, dd, eg, eu, ed,
    ybuf, pbuf, mbuf, nbuf, wide_s, sbuf, dbuf, obuf, rbuf,
    wsem, ysend, yrecv, msend, mrecv, nsend, nrecv, fsend, dsend, drecv, rsend, rrecv,
):
    n, cores = lax.axis_size("ep"), lax.axis_size("tp")
    me, t = lax.axis_index("ep"), lax.axis_index("tp")
    other = 1 - t
    plane = PLANE if n % PLANE == 0 else 1
    depth = n // plane
    zz, q = me // plane, lax.rem(me, plane)
    count, features = resid_ref.shape
    half = count // cores
    batch = n * count

    loads = [
        pltpu.make_async_copy(a, b, wsem.at[i])
        for i, (a, b) in enumerate(
            ((oproj_hbm, oproj), (dg_hbm, dg), (du_hbm, du), (eg_hbm, eg),
             (eu_hbm, eu), (dd_hbm, dd), (ed_hbm, ed))
        )
    ]
    barrier = pltpu.get_barrier_semaphore()

    def greet(k, _):
        peer = lax.rem(me + k, n)
        for core in range(cores):
            pl.semaphore_signal(barrier, inc=1, device_id=(peer, core), device_id_type=MESH)
        return 0

    lax.fori_loop(1, n, greet, 0)
    pl.semaphore_signal(barrier, inc=1, device_id=(me, other), device_id_type=MESH)
    for load in loads:
        load.start()
    ybuf[me] = y_ref[...]
    pl.semaphore_wait(barrier, n * cores - 1)

    def remote(src, dst, send, recv, device):
        return pltpu.make_async_remote_copy(
            src_ref=src, dst_ref=dst, send_sem=send, recv_sem=recv,
            device_id=device, device_id_type=MESH,
        )

    def beside(k):
        return zz * plane + lax.rem(q + k, plane)

    def across(k):
        return lax.rem(zz + k, depth) * plane + q

    def all_gather(first, buf, send, recv, landed):
        for k in range(1, depth):
            peer = across(k)
            remote(first, buf.at[me], send.at[peer], recv.at[me], (peer, t)).start()
        for k in range(1, plane):
            peer = beside(k)
            remote(first, buf.at[me], send.at[peer], recv.at[me], (peer, t)).start()
        landed(me)
        for k in range(1, depth):
            source = across(depth - k)
            remote(buf.at[source], buf.at[source], send.at[source], recv.at[source], (me, other)).wait_recv()
            for i in range(1, plane):
                peer = beside(i)
                slot = (source // plane) * plane + lax.rem(peer, plane)
                remote(buf.at[source], buf.at[source], send.at[slot], recv.at[source], (peer, t)).start()
            landed(source)

        def arrive(level, _):
            base = lax.rem(zz + level, depth) * plane
            for i in range(1, plane):
                source = base + lax.rem(q + i, plane)
                remote(buf.at[source], buf.at[source], send.at[source], recv.at[source], (me, other)).wait_recv()
                landed(source)
            return 0

        lax.fori_loop(0, depth, arrive, 0)

    def drain(first, send):
        def one(k, _):
            peer = lax.rem(me + k, n)
            remote(first, first, send.at[peer], send.at[peer], (me, other)).wait_send()
            return 0

        lax.fori_loop(1, n, one, 0)

    all_gather(y_ref, ybuf, ysend, yrecv, lambda source: None)
    loads[0].wait()
    partial = mm(ybuf[...].reshape(batch, ybuf.shape[2]), oproj[...])
    pbuf[...] = partial.astype(BF16).reshape(pbuf.shape)
    mbuf[t, me] = pbuf[me]

    def scatter(k, _):
        peer = lax.rem(me + k, n)
        for core in range(cores):
            remote(pbuf.at[peer], mbuf.at[t, me], msend.at[core, peer], mrecv.at[t, me], (peer, core)).start()
        return 0

    lax.fori_loop(1, n, scatter, 0)
    remote(pbuf.at[me], mbuf.at[t, me], msend.at[other, me], mrecv.at[t, me], (me, other)).start()

    def collect(k, _):
        peer = lax.rem(me + k, n)
        for core in range(cores):
            remote(pbuf.at[peer], mbuf.at[core, peer], msend.at[core, peer], mrecv.at[core, peer], (me, other)).wait_recv()
        return 0

    lax.fori_loop(1, n, collect, 0)
    remote(pbuf.at[me], mbuf.at[other, me], msend.at[other, me], mrecv.at[other, me], (me, other)).wait_recv()

    mixed = jnp.concatenate(
        [sum(mbuf[core, e].astype(F32) for core in range(cores)) for e in range(n)], axis=1
    )
    widened = (resid_ref[...].astype(F32) + mixed).astype(BF16).astype(F32)
    wide_s[...] = widened
    normed = (
        widened
        * lax.rsqrt(jnp.mean(widened * widened, axis=-1, keepdims=True) + EPSILON)
        * gain_ref[...]
    ).astype(BF16)
    part = features // cores
    for core in range(cores):
        nbuf[core, me] = normed[:, core * part : (core + 1) * part]

    def pass_on(source):
        @pl.when(source != me)
        def _():
            remote(nbuf.at[t, source], nbuf.at[t, source], fsend.at[source], nrecv.at[t, source], (me, other)).start()

    all_gather(nbuf.at[t, me], nbuf.at[t], nsend, nrecv.at[t], pass_on)

    def passed(k, _):
        peer = lax.rem(me + k, n)
        remote(nbuf.at[other, peer], nbuf.at[other, peer], fsend.at[peer], nrecv.at[other, peer], (me, other)).wait_recv()
        return 0

    lax.fori_loop(1, n, passed, 0)

    chunks = [nbuf[core].reshape(batch, part) for core in range(cores)]
    for load in loads[1:5]:
        load.wait()

    def project(w):
        return sum(mm(chunks[core], w[core * part : (core + 1) * part, :]) for core in range(cores))

    score = sum(
        jnp.sum(
            chunks[core].astype(F32) * bgate_ref[:, core * part : (core + 1) * part].astype(F32),
            axis=1, keepdims=True,
        )
        for core in range(cores)
    )
    dense_hidden = (jax.nn.sigmoid(score) * jax.nn.silu(project(dg)) * project(du)).astype(BF16)
    pick = (iota(gw_ref.shape, 1) == me // (n // GROUPS)).astype(F32)
    coarse = jnp.sum(gw_ref[...] * pick, axis=1, keepdims=True)
    mine = (ids_ref[...] == me).astype(F32)
    weight = jnp.sum(mine * (ew_ref[...] * coarse), axis=1, keepdims=True)
    row_hidden = (weight * jax.nn.silu(project(eg.at[0])) * project(eu.at[0])).astype(BF16)
    for load in loads[5:]:
        load.wait()
    step = 512
    for start in range(0, features, step):
        cols = slice(start, start + step)
        block = mm(dense_hidden, dd[:, cols]) + mm(row_hidden, ed[0, :, cols])
        block = block.reshape(n, cores, half, step)
        for core in range(cores):
            sbuf[core, :, :, cols] = block[:, core].astype(BF16)

    def swap(level):
        base = pl.ds(lax.rem(zz + 1 + level, depth) * plane, plane)
        return remote(sbuf.at[other, base], dbuf.at[base], dsend.at[level], drecv.at[level], (me, other))

    for level in range(depth):
        swap(level).start()
    for level in range(depth):
        swap(level).wait_recv()
        base = lax.rem(zz + 1 + level, depth) * plane
        for i in range(plane):
            dest = base + i
            total = sbuf[t, dest].astype(F32) + dbuf[dest].astype(F32)
            obuf[dest] = total.astype(BF16)
            if level < depth - 1:
                remote(obuf.at[dest], rbuf.at[me], rsend.at[dest], rrecv.at[me], (dest, t)).start()
            else:
                @pl.when(dest != me)
                def _():
                    remote(obuf.at[dest], rbuf.at[me], rsend.at[dest], rrecv.at[me], (dest, t)).start()

    total = wide_s[pl.ds(pl.multiple_of(t * half, half), half), :]
    total = total + sbuf[t, me].astype(F32) + dbuf[me].astype(F32)

    def final(k, total):
        peer = lax.rem(me + k, n)
        remote(obuf.at[peer], rbuf.at[peer], rsend.at[peer], rrecv.at[peer], (me, other)).wait_recv()
        return total + rbuf[peer].astype(F32)

    total = lax.fori_loop(1, n, final, total)
    out_ref[...] = total.astype(BF16)
    drain(y_ref, ysend)
    drain(nbuf.at[t, me], nsend)
    drain(nbuf.at[t, me], fsend)
    drain(obuf.at[me], rsend)
    for core in range(cores):
        drain(pbuf.at[me], msend.at[core])
    remote(pbuf.at[me], mbuf.at[t, me], msend.at[other, me], mrecv.at[t, me], (me, other)).wait_send()
    for level in range(depth):
        swap(level).wait_send()


def layer(
    y_out, resid, out_proj, ffn_gain, dense_gate, dense_up, dense_down, branch_gate,
    group_weights, expert_ids, expert_weights, exp_gate, exp_up, exp_down,
):
    n, cores = lax.axis_size("ep"), lax.axis_size("tp")
    count, features = resid.shape
    half = count // cores
    depth = n // PLANE if n % PLANE == 0 else n
    vmem = pl.BlockSpec(memory_space=pltpu.VMEM)
    hbm = pl.BlockSpec(memory_space=pl.ANY)
    weights = (out_proj, dense_gate, dense_up, dense_down, exp_gate, exp_up, exp_down)
    dma = pltpu.SemaphoreType.DMA
    return pl.pallas_call(
        layer_kernel,
        in_specs=[vmem] * 7 + [hbm] * 7,
        out_specs=vmem,
        out_shape=jax.ShapeDtypeStruct((half, features), BF16),
        scratch_shapes=[pltpu.VMEM(w.shape, w.dtype) for w in weights]
        + [
            pltpu.VMEM((n,) + y_out.shape, BF16),
            pltpu.VMEM((n, count, out_proj.shape[1]), BF16),
            pltpu.VMEM((cores, n, count, out_proj.shape[1]), BF16),
            pltpu.VMEM((cores, n, count, features // cores), BF16),
            pltpu.VMEM((count, features), F32),
            pltpu.VMEM((cores, n, half, features), BF16),
            pltpu.VMEM((n, half, features), BF16),
            pltpu.VMEM((n, half, features), BF16),
            pltpu.VMEM((n, half, features), BF16),
            dma((7,)), dma((n,)), dma((n,)), dma((cores, n)), dma((cores, n)),
            dma((n,)), dma((cores, n)), dma((n,)), dma((depth,)), dma((depth,)),
            dma((n,)), dma((n,)),
        ],
        compiler_params=pltpu.CompilerParams(
            collective_id=0, has_side_effects=True, vmem_limit_bytes=60 * 1024 * 1024
        ),
        name="layer_step",
    )(
        y_out, resid, ffn_gain[None], branch_gate[None], group_weights, expert_ids,
        expert_weights, *weights,
    )


def state_update(
    proj_x,
    proj_z,
    proj_bc,
    proj_dt,
    tail_x,
    tail_bc,
    taps_x,
    taps_bc,
    ssm_state,
    dt_bias,
    decay_log,
    group_gain,
):
    window_x = jnp.concatenate([tail_x, proj_x[:, None]], axis=1).astype(jnp.float32)
    conv_x = jax.nn.silu(jnp.sum(window_x * taps_x.astype(jnp.float32)[None], axis=1))
    window_bc = jnp.concatenate([tail_bc, proj_bc[:, None]], axis=1).astype(jnp.float32)
    conv_bc = jax.nn.silu(jnp.sum(window_bc * taps_bc.astype(jnp.float32)[None], axis=1))
    count = proj_x.shape[0]
    heads = proj_dt.shape[1]
    x_heads = conv_x.reshape(count, heads, HEAD_P)
    grouped_bc = conv_bc.reshape(count, 2, heads // HPG, NSTATE)
    input_heads = jnp.repeat(grouped_bc[:, 0], HPG, axis=1)
    read_heads = jnp.repeat(grouped_bc[:, 1], HPG, axis=1)
    step_size = jax.nn.softplus(proj_dt.astype(jnp.float32) + dt_bias)
    decay = jnp.exp(-step_size * jnp.exp(decay_log))
    state = ssm_state.reshape(count, heads, HEAD_P, NSTATE)
    fresh = (step_size[:, :, None] * x_heads)[:, :, :, None] * input_heads[:, :, None, :]
    new_state = decay[:, :, None, None] * state + fresh
    readout = jnp.sum(new_state * read_heads[:, :, None, :], axis=-1)
    gated = readout.reshape(count, heads * HEAD_P) * jax.nn.silu(proj_z.astype(jnp.float32))
    grouped = gated.reshape(count, heads // HPG, HPG * HEAD_P)
    grouped = grouped * lax.rsqrt(jnp.mean(grouped * grouped, axis=-1, keepdims=True) + EPSILON)
    y_out = (grouped.reshape(count, heads * HEAD_P) * group_gain).astype(jnp.bfloat16)
    return (y_out, new_state.reshape(count, heads, HEAD_P * NSTATE))


def shards(
    resid,
    proj_x,
    proj_z,
    proj_bc,
    proj_dt,
    tail_x,
    tail_bc,
    taps_x,
    taps_bc,
    ssm_state,
    dt_bias,
    decay_log,
    group_gain,
    out_proj,
    ffn_gain,
    dense_gate,
    dense_up,
    dense_down,
    branch_gate,
    group_weights,
    expert_ids,
    expert_weights,
    exp_gate,
    exp_up,
    exp_down,
):
    if out_proj.shape[1] % 128 == 0 and lax.axis_size("tp") == 2:
        y_out, new_state = state_step(
            proj_x, proj_z, proj_bc, proj_dt, tail_x, tail_bc, taps_x, taps_bc, ssm_state,
            dt_bias, decay_log, group_gain,
        )
        out = layer(
            y_out, resid, out_proj, ffn_gain, dense_gate, dense_up, dense_down, branch_gate,
            group_weights, expert_ids, expert_weights, exp_gate, exp_up, exp_down,
        )
        return (out, new_state)
    y_out, new_state = state_update(
        proj_x,
        proj_z,
        proj_bc,
        proj_dt,
        tail_x,
        tail_bc,
        taps_x,
        taps_bc,
        ssm_state,
        dt_bias,
        decay_log,
        group_gain,
    )
    partial_value = jnp.dot(
        lax.all_gather(y_out, "ep", axis=0, tiled=True),
        out_proj,
        preferred_element_type=jnp.float32,
    )
    partial_value = lax.all_to_all(
        partial_value.astype(jnp.bfloat16), "ep", split_axis=0, concat_axis=1, tiled=True
    ).astype(partial_value.dtype)
    mixed = lax.psum(partial_value.astype(jnp.bfloat16), "tp").astype(jnp.float32)
    resid_new = (resid.astype(jnp.float32) + mixed).astype(jnp.bfloat16)
    widened = resid_new.astype(jnp.float32)
    normed = (
        widened
        * lax.rsqrt(jnp.mean(widened * widened, axis=-1, keepdims=True) + EPSILON)
        * ffn_gain
    ).astype(jnp.bfloat16)
    gathered = lax.all_gather(normed, "ep", axis=0, tiled=True)
    score = jnp.dot(gathered, branch_gate, preferred_element_type=jnp.float32)
    dense_pre = jnp.dot(gathered, dense_gate, preferred_element_type=jnp.float32)
    dense_lin = jnp.dot(gathered, dense_up, preferred_element_type=jnp.float32)
    dense_hidden = (jax.nn.sigmoid(score)[:, None] * jax.nn.silu(dense_pre) * dense_lin).astype(
        jnp.bfloat16
    )
    experts = lax.axis_size("ep")
    expert_own = lax.axis_index("ep")
    cores = lax.axis_size("tp")
    core_index = lax.axis_index("tp")
    batch = gathered.shape[0]
    rows_each = batch // experts
    half_rows = rows_each // cores
    pairs = rows_each * TOPK
    capacity = (pairs + experts - 1) // experts + 1
    group_size = experts // GROUPS
    levels = jnp.arange(1, capacity + 1, dtype=jnp.int32)
    pair_row = jnp.arange(pairs, dtype=jnp.int32) // TOPK
    pick = (jnp.arange(GROUPS, dtype=jnp.int32) == expert_own // group_size).astype(jnp.float32)
    coarse = jnp.sum(group_weights * pick[None], axis=1)
    pair_weight = (expert_weights * coarse[:, None]).reshape(experts, pairs)
    hits = (expert_ids.reshape(experts, pairs) == expert_own).astype(jnp.int32)
    ranks = jnp.cumsum(hits, axis=1, dtype=jnp.int32)
    select = hits[:, None, :] * (ranks[:, None, :] == levels[None, :, None]).astype(jnp.int32)
    local_row = jnp.sum(select * pair_row[None, None, :], axis=-1, dtype=jnp.int32)
    filled = jnp.sum(select, axis=-1, dtype=jnp.int32).reshape(-1)
    slot_weight = jnp.sum(select.astype(jnp.float32) * pair_weight[:, None, :], axis=-1).reshape(-1)
    row_index = (local_row + jnp.arange(experts, dtype=jnp.int32)[:, None] * rows_each).reshape(-1)
    slot_rows = jnp.take(gathered, row_index, axis=0)
    slot_pre = jnp.dot(slot_rows, exp_gate[0], preferred_element_type=jnp.float32)
    slot_lin = jnp.dot(slot_rows, exp_up[0], preferred_element_type=jnp.float32)
    slot_hidden = (slot_weight[:, None] * jax.nn.silu(slot_pre) * slot_lin).astype(jnp.bfloat16)
    placing = (jnp.arange(batch, dtype=jnp.int32)[:, None] == row_index[None, :]) & (
        filled[None, :] > 0
    )
    row_hidden = jnp.dot(
        placing.astype(jnp.bfloat16), slot_hidden, preferred_element_type=jnp.float32
    ).astype(jnp.bfloat16)
    joined = jnp.concatenate([dense_hidden, row_hidden], axis=1)
    down_all = jnp.concatenate([dense_down, exp_down[0]], axis=0)
    inner_width = joined.shape[1]
    ordered = (
        joined.reshape(experts, cores, half_rows, inner_width)
        .transpose(1, 0, 2, 3)
        .reshape(batch, inner_width)
    )
    halved = lax.psum_scatter(
        jnp.dot(ordered, down_all, preferred_element_type=jnp.float32).astype(jnp.bfloat16),
        "tp",
        scatter_dimension=0,
        tiled=True,
    ).astype(jnp.float32)
    branch = lax.psum_scatter(halved, "ep", scatter_dimension=0, tiled=True)
    own_rows = lax.dynamic_slice_in_dim(widened, core_index * half_rows, half_rows, 0)
    out = (own_rows + branch).astype(jnp.bfloat16)
    return (out, new_state)


def solution(mesh):
    return jax.shard_map(
        shards,
        mesh=mesh,
        in_specs=(
            P("ep", None),
            P("ep", "tp"),
            P("ep", "tp"),
            P("ep", None, "tp"),
            P("ep", "tp"),
            P("ep", None, "tp"),
            P("ep", None, None, "tp"),
            P(None, "tp"),
            P(None, None, "tp"),
            P("ep", "tp", None),
            P("tp"),
            P("tp"),
            P("tp"),
            P("tp", "ep"),
            P(),
            P(None, ("ep", "tp")),
            P(None, ("ep", "tp")),
            P(("ep", "tp"), None),
            P(),
            P(),
            P(),
            P(),
            P("ep", None, "tp"),
            P("ep", None, "tp"),
            P("ep", "tp", None),
        ),
        out_specs=(P(("ep", "tp"), None), P("ep", "tp", None)),
        check_vma=False,
    )
```

```python
import functools

import jax
import jax.numpy as jnp
from jax import lax
from jax.experimental import pallas as pl
from jax.experimental.pallas import tpu as pltpu
from jax.sharding import PartitionSpec as P

HEAD_P = 64
NSTATE = 64
GROUPS = 4
TOPK = 6
HPG = 4


EPSILON = 1e-06
LANES = 512
PLANE = 4
MESH = pl.DeviceIdType.MESH
F32 = jnp.float32
BF16 = jnp.bfloat16


def mm(a, b):
    return jnp.dot(a, b, preferred_element_type=F32)


def iota(shape, dim):
    return lax.broadcasted_iota(jnp.int32, shape, dim)


def one_hot(cond):
    return cond.astype(F32).astype(BF16)


def state_kernel(
    x_ref, z_ref, bc_ref, tail_x_ref, tail_bc_ref, taps_x_ref, taps_bc_ref, dt_ref, bias_ref, log_ref, gain_ref, state_ref,
    y_ref, new_ref, xs, inp_s, rd_s, decay_s, acc,
):
    j = pl.program_id(0)
    count, heads = dt_ref.shape
    rows = count * heads
    inner = heads * HEAD_P
    groups = heads // HPG

    def head_mask(lanes, per):
        head = lax.rem(iota((rows, lanes), 0), heads)
        return head // (HPG if per == groups else 1) == iota((rows, lanes), 1) // (lanes // per)

    @pl.when(j == 0)
    def _():
        spread = one_hot(iota((rows, count), 0) // heads == iota((rows, count), 1))
        taps = taps_x_ref.shape[0]
        taps_x = taps_x_ref[...].astype(F32)
        conv_x = x_ref[...].astype(F32) * taps_x[taps - 1 : taps]
        for w in range(taps - 1):
            conv_x = conv_x + tail_x_ref[w].astype(F32) * taps_x[w : w + 1]
        conv_x = jax.nn.silu(conv_x)
        conv_bc = []
        for i in range(2):
            conv = bc_ref[:, i, :].astype(F32) * taps_bc_ref[taps - 1, i : i + 1, :].astype(F32)
            for w in range(taps - 1):
                conv = conv + tail_bc_ref[:, w, i, :].astype(F32) * taps_bc_ref[w, i : i + 1, :].astype(F32)
            conv_bc.append(jax.nn.silu(conv))
        dt = mm(spread, dt_ref[...])
        step = jax.nn.softplus(dt + bias_ref[...])
        decay = jnp.exp(-step * jnp.exp(log_ref[...]))
        own = head_mask(heads, heads)
        step_col = jnp.sum(jnp.where(own, step, 0.0), axis=1, keepdims=True)
        decay_s[...] = jnp.sum(jnp.where(own, decay, 0.0), axis=1, keepdims=True)
        xr = mm(spread, conv_x.astype(BF16))
        xr = jnp.where(head_mask(inner, heads), xr, 0.0).astype(BF16)
        fold = one_hot(lax.rem(iota((inner, HEAD_P), 0), HEAD_P) == iota((inner, HEAD_P), 1))
        xs[...] = mm(xr, fold).astype(BF16)
        width = groups * NSTATE
        gmask = head_mask(width, groups)
        twice = one_hot(
            lax.rem(iota((width, 2 * NSTATE), 0), NSTATE)
            == lax.rem(iota((width, 2 * NSTATE), 1), NSTATE)
        )
        ir = jnp.where(gmask, mm(spread, conv_bc[0].astype(BF16)), 0.0).astype(BF16)
        inp_s[...] = mm(ir, twice) * step_col
        rr = jnp.where(gmask, mm(spread, conv_bc[1].astype(BF16)), 0.0).astype(BF16)
        rd_s[...] = mm(rr, twice)
        acc[...] = jnp.zeros_like(acc)

    lanes = state_ref.shape[1]
    tiles = lanes // (2 * NSTATE)
    expand = one_hot(
        iota((HEAD_P, lanes), 0) == (iota((HEAD_P, lanes), 1) + j * lanes) // NSTATE
    )
    collect = one_hot(
        iota((lanes, HEAD_P), 1) == (iota((lanes, HEAD_P), 0) + j * lanes) // NSTATE
    )
    fresh = mm(xs[...], expand) * jnp.concatenate([inp_s[...]] * tiles, axis=1)
    new = decay_s[...] * state_ref[...] + fresh
    new_ref[...] = new
    prod = (new * jnp.concatenate([rd_s[...]] * tiles, axis=1)).astype(BF16)
    acc[...] += mm(prod, collect)

    @pl.when(j == pl.num_programs(0) - 1)
    def _():
        unfold = one_hot(lax.rem(iota((HEAD_P, inner), 1), HEAD_P) == iota((HEAD_P, inner), 0))
        gatherer = one_hot(iota((count, rows), 1) // heads == iota((count, rows), 0))
        mask = head_mask(inner, heads)
        high = acc[...].astype(BF16)
        low = (acc[...] - high.astype(F32)).astype(BF16)
        read = jnp.zeros((count, inner), F32)
        for piece in (high, low):
            wide = jnp.where(mask, mm(piece, unfold), 0.0).astype(BF16)
            read = read + mm(gatherer, wide)
        gated = read * jax.nn.silu(z_ref[...].astype(F32))
        size = HPG * HEAD_P
        for g in range(groups):
            cols = slice(g * size, (g + 1) * size)
            part = gated[:, cols]
            part = part * lax.rsqrt(jnp.mean(part * part, axis=-1, keepdims=True) + EPSILON)
            y_ref[:, cols] = (part * gain_ref[:, cols]).astype(BF16)


def state_step(
    proj_x, proj_z, proj_bc, proj_dt, tail_x, tail_bc, taps_x, taps_bc, ssm_state,
    dt_bias, decay_log, group_gain,
):
    count, heads, width = ssm_state.shape
    rows = count * heads
    full = lambda a: pl.BlockSpec(a.shape, lambda j: (0,) * a.ndim)
    small = (
        proj_x, proj_z, proj_bc, tail_x.transpose(1, 0, 2), tail_bc, taps_x, taps_bc, proj_dt,
        dt_bias[None], decay_log[None], group_gain[None],
    )
    block = pl.BlockSpec((rows, LANES), lambda j: (0, j))
    y_out, new_state = pl.pallas_call(
        state_kernel,
        grid=(width // LANES,),
        in_specs=[full(a) for a in small] + [block],
        out_specs=[pl.BlockSpec((count, heads * HEAD_P), lambda j: (0, 0)), block],
        out_shape=[
            jax.ShapeDtypeStruct((count, heads * HEAD_P), BF16),
            jax.ShapeDtypeStruct((rows, width), F32),
        ],
        scratch_shapes=[
            pltpu.VMEM((rows, HEAD_P), BF16),
            pltpu.VMEM((rows, 2 * NSTATE), F32),
            pltpu.VMEM((rows, 2 * NSTATE), F32),
            pltpu.VMEM((rows, 1), F32),
            pltpu.VMEM((rows, HEAD_P), F32),
        ],
        name="state_step",
    )(*small, ssm_state.reshape(rows, width))
    return y_out, new_state.reshape(count, heads, width)


def layer_kernel(
    y_ref, resid_ref, gain_ref, bgate_ref, gw_ref, ids_ref, ew_ref,
    oproj_hbm, dg_hbm, du_hbm, dd_hbm, eg_hbm, eu_hbm, ed_hbm,
    out_ref,
    oproj, dg, du, dd, eg, eu, ed,
    ybuf, pbuf, mbuf, nbuf, wide_s, sbuf, dbuf, obuf, rbuf, zbuf, hbuf,
    wsem, ysend, yrecv, msend, mrecv, nsend, nrecv, fsend, dsend, drecv, rsend, rrecv, zsend, zrecv,
):
    n, cores = lax.axis_size("ep"), lax.axis_size("tp")
    me, t = lax.axis_index("ep"), lax.axis_index("tp")
    other = 1 - t
    plane = PLANE if n % PLANE == 0 else 1
    depth = n // plane
    zz, q = me // plane, lax.rem(me, plane)
    count, features = resid_ref.shape
    half = count // cores
    batch = n * count

    loads = [
        pltpu.make_async_copy(a, b, wsem.at[i])
        for i, (a, b) in enumerate(
            ((oproj_hbm, oproj), (dg_hbm, dg), (du_hbm, du), (eg_hbm, eg),
             (eu_hbm, eu), (dd_hbm, dd), (ed_hbm, ed))
        )
    ]
    barrier = pltpu.get_barrier_semaphore()

    def greet(k, _):
        peer = lax.rem(me + k, n)
        for core in range(cores):
            pl.semaphore_signal(barrier, inc=1, device_id=(peer, core), device_id_type=MESH)
        return 0

    lax.fori_loop(1, n, greet, 0)
    pl.semaphore_signal(barrier, inc=1, device_id=(me, other), device_id_type=MESH)
    for load in loads:
        load.start()
    ybuf[me] = y_ref[...]
    pl.semaphore_wait(barrier, n * cores - 1)

    def remote(src, dst, send, recv, device):
        return pltpu.make_async_remote_copy(
            src_ref=src, dst_ref=dst, send_sem=send, recv_sem=recv,
            device_id=device, device_id_type=MESH,
        )

    def beside(k):
        return zz * plane + lax.rem(q + k, plane)

    def across(k):
        return lax.rem(zz + k, depth) * plane + q

    def all_gather(first, buf, send, recv, landed):
        for k in range(1, depth):
            peer = across(k)
            remote(first, buf.at[me], send.at[peer], recv.at[me], (peer, t)).start()
        for k in range(1, plane):
            peer = beside(k)
            remote(first, buf.at[me], send.at[peer], recv.at[me], (peer, t)).start()
        landed(me)
        for k in range(1, depth):
            source = across(depth - k)
            remote(buf.at[source], buf.at[source], send.at[source], recv.at[source], (me, other)).wait_recv()
            for i in range(1, plane):
                peer = beside(i)
                slot = (source // plane) * plane + lax.rem(peer, plane)
                remote(buf.at[source], buf.at[source], send.at[slot], recv.at[source], (peer, t)).start()
            landed(source)

        def arrive(level, _):
            base = lax.rem(zz + level, depth) * plane
            for i in range(1, plane):
                source = base + lax.rem(q + i, plane)
                remote(buf.at[source], buf.at[source], send.at[source], recv.at[source], (me, other)).wait_recv()
                landed(source)
            return 0

        lax.fori_loop(0, depth, arrive, 0)

    def drain(first, send):
        def one(k, _):
            peer = lax.rem(me + k, n)
            remote(first, first, send.at[peer], send.at[peer], (me, other)).wait_send()
            return 0

        lax.fori_loop(1, n, one, 0)

    all_gather(y_ref, ybuf, ysend, yrecv, lambda source: None)
    loads[0].wait()
    partial = mm(ybuf[...].reshape(batch, ybuf.shape[2]), oproj[...])
    pbuf[...] = partial.astype(BF16).reshape(pbuf.shape)
    mbuf[t, me] = pbuf[me]

    def scatter(k, _):
        peer = lax.rem(me + k, n)
        for core in range(cores):
            remote(pbuf.at[peer], mbuf.at[t, me], msend.at[core, peer], mrecv.at[t, me], (peer, core)).start()
        return 0

    lax.fori_loop(1, n, scatter, 0)
    remote(pbuf.at[me], mbuf.at[t, me], msend.at[other, me], mrecv.at[t, me], (me, other)).start()

    def collect(k, _):
        peer = lax.rem(me + k, n)
        for core in range(cores):
            remote(pbuf.at[peer], mbuf.at[core, peer], msend.at[core, peer], mrecv.at[core, peer], (me, other)).wait_recv()
        return 0

    lax.fori_loop(1, n, collect, 0)
    remote(pbuf.at[me], mbuf.at[other, me], msend.at[other, me], mrecv.at[other, me], (me, other)).wait_recv()

    mixed = jnp.concatenate(
        [sum(mbuf[core, e].astype(F32) for core in range(cores)) for e in range(n)], axis=1
    )
    widened = (resid_ref[...].astype(F32) + mixed).astype(BF16).astype(F32)
    wide_s[...] = widened
    normed = (
        widened
        * lax.rsqrt(jnp.mean(widened * widened, axis=-1, keepdims=True) + EPSILON)
        * gain_ref[...]
    ).astype(BF16)
    part = features // cores
    for core in range(cores):
        nbuf[core, me] = normed[:, core * part : (core + 1) * part]

    def pass_on(source):
        @pl.when(source != me)
        def _():
            remote(nbuf.at[t, source], nbuf.at[t, source], fsend.at[source], nrecv.at[t, source], (me, other)).start()

    all_gather(nbuf.at[t, me], nbuf.at[t], nsend, nrecv.at[t], pass_on)

    def passed(k, _):
        peer = lax.rem(me + k, n)
        remote(nbuf.at[other, peer], nbuf.at[other, peer], fsend.at[peer], nrecv.at[other, peer], (me, other)).wait_recv()
        return 0

    lax.fori_loop(1, n, passed, 0)

    chunks = [nbuf[core].reshape(batch, part) for core in range(cores)]
    for load in loads[1:5]:
        load.wait()

    def project(w):
        return sum(mm(chunks[core], w[core * part : (core + 1) * part, :]) for core in range(cores))

    bgate = bgate_ref[...].astype(F32)
    bgate = jnp.concatenate([bgate[i : i + 1] for i in range(bgate.shape[0])], axis=1)
    score = sum(
        jnp.sum(
            chunks[core].astype(F32) * bgate[:, core * part : (core + 1) * part],
            axis=1, keepdims=True,
        )
        for core in range(cores)
    )
    dense_hidden = (jax.nn.sigmoid(score) * jax.nn.silu(project(dg)) * project(du)).astype(BF16)
    pick = (iota(gw_ref.shape, 0) == me // (n // GROUPS)).astype(F32)
    coarse = jnp.sum(gw_ref[...] * pick, axis=0, keepdims=True)
    mine = (ids_ref[...] == me).astype(F32)
    weight_row = jnp.sum(mine * (ew_ref[...] * coarse), axis=0, keepdims=True)
    diagonal = iota((batch, batch), 0) == iota((batch, batch), 1)
    weight = jnp.sum(jnp.where(diagonal, weight_row, 0.0), axis=1, keepdims=True)
    row_hidden = (weight * jax.nn.silu(project(eg.at[0])) * project(eu.at[0])).astype(BF16)
    for load in loads[5:]:
        load.wait()
    step = 512
    for start in range(0, features, step):
        cols = slice(start, start + step)
        block = mm(dense_hidden, dd[:, cols]) + mm(row_hidden, ed[0, :, cols])
        block = block.reshape(n, cores, half, step)
        for core in range(cores):
            sbuf[core, :, :, cols] = block[:, core].astype(BF16)

    def swap(level):
        base = pl.ds(lax.rem(zz + 1 + level, depth) * plane, plane)
        return remote(sbuf.at[other, base], dbuf.at[base], dsend.at[level], drecv.at[level], (me, other))

    for level in range(depth):
        swap(level).start()
    def in_plane(level, i):
        base = lax.rem(zz + 1 + level, depth) * plane
        peer = lax.rem(q + i, plane)
        return remote(
            obuf.at[base + peer], rbuf.at[base + q], rsend.at[base + peer], rrecv.at[base + q],
            (zz * plane + peer, t),
        )

    def summed(dest):
        return sbuf[t, dest].astype(F32) + dbuf[dest].astype(F32)

    def to_owner(level):
        owner = lax.rem(zz + 1 + level, depth)
        return remote(
            zbuf.at[owner], hbuf.at[zz], zsend.at[owner], zrecv.at[zz], (owner * plane + q, t)
        )

    def finish(level):
        owner = lax.rem(zz + 1 + level, depth)
        base = owner * plane
        total = summed(base + q)
        for i in range(1, plane):
            source = base + lax.rem(q + i, plane)
            remote(rbuf.at[source], rbuf.at[source], rsend.at[source], rrecv.at[source], (me, other)).wait_recv()
            total = total + rbuf[source].astype(F32)
        if level < depth - 1:
            zbuf[owner] = total.astype(BF16)
            to_owner(level).start()
        return total

    for level in range(depth):
        swap(level).wait_recv()
        base = lax.rem(zz + 1 + level, depth) * plane
        for i in range(1, plane):
            dest = base + lax.rem(q + i, plane)
            obuf[dest] = summed(dest).astype(BF16)
            in_plane(level, i).start()
        if level > 0:
            finish(level - 1)
    total = finish(depth - 1) + wide_s[pl.ds(pl.multiple_of(t * half, half), half), :]
    for k in range(1, depth):
        source = lax.rem(zz + depth - k, depth)
        remote(hbuf.at[source], hbuf.at[source], zsend.at[source], zrecv.at[source], (me, other)).wait_recv()
        total = total + hbuf[source].astype(F32)
    out_ref[...] = total.astype(BF16)
    drain(y_ref, ysend)
    drain(nbuf.at[t, me], nsend)
    drain(nbuf.at[t, me], fsend)
    for core in range(cores):
        drain(pbuf.at[me], msend.at[core])
    remote(pbuf.at[me], mbuf.at[t, me], msend.at[other, me], mrecv.at[t, me], (me, other)).wait_send()
    for level in range(depth):
        swap(level).wait_send()
        for i in range(1, plane):
            in_plane(level, i).wait_send()
        if level < depth - 1:
            to_owner(level).wait_send()


def layer(
    y_out, resid, out_proj, ffn_gain, dense_gate, dense_up, dense_down, branch_gate,
    group_weights, expert_ids, expert_weights, exp_gate, exp_up, exp_down,
):
    n, cores = lax.axis_size("ep"), lax.axis_size("tp")
    count, features = resid.shape
    half = count // cores
    depth = n // PLANE if n % PLANE == 0 else n
    vmem = pl.BlockSpec(memory_space=pltpu.VMEM)
    hbm = pl.BlockSpec(memory_space=pl.ANY)
    weights = (out_proj, dense_gate, dense_up, dense_down, exp_gate, exp_up, exp_down)
    dma = pltpu.SemaphoreType.DMA
    return pl.pallas_call(
        layer_kernel,
        in_specs=[vmem] * 7 + [hbm] * 7,
        out_specs=vmem,
        out_shape=jax.ShapeDtypeStruct((half, features), BF16),
        scratch_shapes=[pltpu.VMEM(w.shape, w.dtype) for w in weights]
        + [
            pltpu.VMEM((n,) + y_out.shape, BF16),
            pltpu.VMEM((n, count, out_proj.shape[1]), BF16),
            pltpu.VMEM((cores, n, count, out_proj.shape[1]), BF16),
            pltpu.VMEM((cores, n, count, features // cores), BF16),
            pltpu.VMEM((count, features), F32),
            pltpu.VMEM((cores, n, half, features), BF16),
            pltpu.VMEM((n, half, features), BF16),
            pltpu.VMEM((n, half, features), BF16),
            pltpu.VMEM((n, half, features), BF16),
            pltpu.VMEM((depth, half, features), BF16),
            pltpu.VMEM((depth, half, features), BF16),
            dma((7,)), dma((n,)), dma((n,)), dma((cores, n)), dma((cores, n)),
            dma((n,)), dma((cores, n)), dma((n,)), dma((depth,)), dma((depth,)),
            dma((n,)), dma((n,)), dma((depth,)), dma((depth,)),
        ],
        compiler_params=pltpu.CompilerParams(
            collective_id=0, has_side_effects=True, vmem_limit_bytes=60 * 1024 * 1024
        ),
        name="layer_step",
    )(
        y_out, resid, ffn_gain[None], branch_gate.reshape(-1, 128), group_weights.T, expert_ids.T,
        expert_weights.T, *weights,
    )


def state_update(
    proj_x,
    proj_z,
    proj_bc,
    proj_dt,
    tail_x,
    tail_bc,
    taps_x,
    taps_bc,
    ssm_state,
    dt_bias,
    decay_log,
    group_gain,
):
    window_x = jnp.concatenate([tail_x, proj_x[:, None]], axis=1).astype(jnp.float32)
    conv_x = jax.nn.silu(jnp.sum(window_x * taps_x.astype(jnp.float32)[None], axis=1))
    window_bc = jnp.concatenate([tail_bc, proj_bc[:, None]], axis=1).astype(jnp.float32)
    conv_bc = jax.nn.silu(jnp.sum(window_bc * taps_bc.astype(jnp.float32)[None], axis=1))
    count = proj_x.shape[0]
    heads = proj_dt.shape[1]
    x_heads = conv_x.reshape(count, heads, HEAD_P)
    grouped_bc = conv_bc.reshape(count, 2, heads // HPG, NSTATE)
    input_heads = jnp.repeat(grouped_bc[:, 0], HPG, axis=1)
    read_heads = jnp.repeat(grouped_bc[:, 1], HPG, axis=1)
    step_size = jax.nn.softplus(proj_dt.astype(jnp.float32) + dt_bias)
    decay = jnp.exp(-step_size * jnp.exp(decay_log))
    state = ssm_state.reshape(count, heads, HEAD_P, NSTATE)
    fresh = (step_size[:, :, None] * x_heads)[:, :, :, None] * input_heads[:, :, None, :]
    new_state = decay[:, :, None, None] * state + fresh
    readout = jnp.sum(new_state * read_heads[:, :, None, :], axis=-1)
    gated = readout.reshape(count, heads * HEAD_P) * jax.nn.silu(proj_z.astype(jnp.float32))
    grouped = gated.reshape(count, heads // HPG, HPG * HEAD_P)
    grouped = grouped * lax.rsqrt(jnp.mean(grouped * grouped, axis=-1, keepdims=True) + EPSILON)
    y_out = (grouped.reshape(count, heads * HEAD_P) * group_gain).astype(jnp.bfloat16)
    return (y_out, new_state.reshape(count, heads, HEAD_P * NSTATE))


def shards(
    resid,
    proj_x,
    proj_z,
    proj_bc,
    proj_dt,
    tail_x,
    tail_bc,
    taps_x,
    taps_bc,
    ssm_state,
    dt_bias,
    decay_log,
    group_gain,
    out_proj,
    ffn_gain,
    dense_gate,
    dense_up,
    dense_down,
    branch_gate,
    group_weights,
    expert_ids,
    expert_weights,
    exp_gate,
    exp_up,
    exp_down,
):
    if out_proj.shape[1] % 128 == 0 and lax.axis_size("tp") == 2:
        y_out, new_state = state_step(
            proj_x, proj_z, proj_bc, proj_dt, tail_x, tail_bc, taps_x, taps_bc, ssm_state,
            dt_bias, decay_log, group_gain,
        )
        out = layer(
            y_out, resid, out_proj, ffn_gain, dense_gate, dense_up, dense_down, branch_gate,
            group_weights, expert_ids, expert_weights, exp_gate, exp_up, exp_down,
        )
        return (out, new_state)
    y_out, new_state = state_update(
        proj_x,
        proj_z,
        proj_bc,
        proj_dt,
        tail_x,
        tail_bc,
        taps_x,
        taps_bc,
        ssm_state,
        dt_bias,
        decay_log,
        group_gain,
    )
    partial_value = jnp.dot(
        lax.all_gather(y_out, "ep", axis=0, tiled=True),
        out_proj,
        preferred_element_type=jnp.float32,
    )
    partial_value = lax.all_to_all(
        partial_value.astype(jnp.bfloat16), "ep", split_axis=0, concat_axis=1, tiled=True
    ).astype(partial_value.dtype)
    mixed = lax.psum(partial_value.astype(jnp.bfloat16), "tp").astype(jnp.float32)
    resid_new = (resid.astype(jnp.float32) + mixed).astype(jnp.bfloat16)
    widened = resid_new.astype(jnp.float32)
    normed = (
        widened
        * lax.rsqrt(jnp.mean(widened * widened, axis=-1, keepdims=True) + EPSILON)
        * ffn_gain
    ).astype(jnp.bfloat16)
    gathered = lax.all_gather(normed, "ep", axis=0, tiled=True)
    score = jnp.dot(gathered, branch_gate, preferred_element_type=jnp.float32)
    dense_pre = jnp.dot(gathered, dense_gate, preferred_element_type=jnp.float32)
    dense_lin = jnp.dot(gathered, dense_up, preferred_element_type=jnp.float32)
    dense_hidden = (jax.nn.sigmoid(score)[:, None] * jax.nn.silu(dense_pre) * dense_lin).astype(
        jnp.bfloat16
    )
    experts = lax.axis_size("ep")
    expert_own = lax.axis_index("ep")
    cores = lax.axis_size("tp")
    core_index = lax.axis_index("tp")
    batch = gathered.shape[0]
    rows_each = batch // experts
    half_rows = rows_each // cores
    pairs = rows_each * TOPK
    capacity = (pairs + experts - 1) // experts + 1
    group_size = experts // GROUPS
    levels = jnp.arange(1, capacity + 1, dtype=jnp.int32)
    pair_row = jnp.arange(pairs, dtype=jnp.int32) // TOPK
    pick = (jnp.arange(GROUPS, dtype=jnp.int32) == expert_own // group_size).astype(jnp.float32)
    coarse = jnp.sum(group_weights * pick[None], axis=1)
    pair_weight = (expert_weights * coarse[:, None]).reshape(experts, pairs)
    hits = (expert_ids.reshape(experts, pairs) == expert_own).astype(jnp.int32)
    ranks = jnp.cumsum(hits, axis=1, dtype=jnp.int32)
    select = hits[:, None, :] * (ranks[:, None, :] == levels[None, :, None]).astype(jnp.int32)
    local_row = jnp.sum(select * pair_row[None, None, :], axis=-1, dtype=jnp.int32)
    filled = jnp.sum(select, axis=-1, dtype=jnp.int32).reshape(-1)
    slot_weight = jnp.sum(select.astype(jnp.float32) * pair_weight[:, None, :], axis=-1).reshape(-1)
    row_index = (local_row + jnp.arange(experts, dtype=jnp.int32)[:, None] * rows_each).reshape(-1)
    slot_rows = jnp.take(gathered, row_index, axis=0)
    slot_pre = jnp.dot(slot_rows, exp_gate[0], preferred_element_type=jnp.float32)
    slot_lin = jnp.dot(slot_rows, exp_up[0], preferred_element_type=jnp.float32)
    slot_hidden = (slot_weight[:, None] * jax.nn.silu(slot_pre) * slot_lin).astype(jnp.bfloat16)
    placing = (jnp.arange(batch, dtype=jnp.int32)[:, None] == row_index[None, :]) & (
        filled[None, :] > 0
    )
    row_hidden = jnp.dot(
        placing.astype(jnp.bfloat16), slot_hidden, preferred_element_type=jnp.float32
    ).astype(jnp.bfloat16)
    joined = jnp.concatenate([dense_hidden, row_hidden], axis=1)
    down_all = jnp.concatenate([dense_down, exp_down[0]], axis=0)
    inner_width = joined.shape[1]
    ordered = (
        joined.reshape(experts, cores, half_rows, inner_width)
        .transpose(1, 0, 2, 3)
        .reshape(batch, inner_width)
    )
    halved = lax.psum_scatter(
        jnp.dot(ordered, down_all, preferred_element_type=jnp.float32).astype(jnp.bfloat16),
        "tp",
        scatter_dimension=0,
        tiled=True,
    ).astype(jnp.float32)
    branch = lax.psum_scatter(halved, "ep", scatter_dimension=0, tiled=True)
    own_rows = lax.dynamic_slice_in_dim(widened, core_index * half_rows, half_rows, 0)
    out = (own_rows + branch).astype(jnp.bfloat16)
    return (out, new_state)


def solution(mesh):
    return jax.shard_map(
        shards,
        mesh=mesh,
        in_specs=(
            P("ep", None),
            P("ep", "tp"),
            P("ep", "tp"),
            P("ep", None, "tp"),
            P("ep", "tp"),
            P("ep", None, "tp"),
            P("ep", None, None, "tp"),
            P(None, "tp"),
            P(None, None, "tp"),
            P("ep", "tp", None),
            P("tp"),
            P("tp"),
            P("tp"),
            P("tp", "ep"),
            P(),
            P(None, ("ep", "tp")),
            P(None, ("ep", "tp")),
            P(("ep", "tp"), None),
            P(),
            P(),
            P(),
            P(),
            P("ep", None, "tp"),
            P("ep", None, "tp"),
            P("ep", "tp", None),
        ),
        out_specs=(P(("ep", "tp"), None), P("ep", "tp", None)),
        check_vma=False,
    )
```
